256 devices in a mesh: ep: 64 (over z, x, core), tp: 4 (over y).
Axes of the slice: x: 4, y: 4, z: 8, core: 2. Of those that a mesh axis runs over, the one named last changes fastest.
Arguments:
- queries: bfloat16 [32768, 2048], P('ep', 'tp'), may hold values from -6 to 6
- keys_values: bfloat16 [32768, 4, 128], P('ep', 'tp'), may hold values from -12 to 12
- sinks: float32 [32], P('tp'), may hold values from 1 to 5
- tokens_b: bfloat16 [32768, 2048], P(('ep', 'tp')), may hold values from -6 to 6
- norm_gain: float32 [2048], replicated, may hold values from 0.1 to 1.9
- routes: int32 [32768, 2], P(('ep', 'tp')), may hold values from 0 to 63, all different within a row; in each aligned block of 128 rows (0 to 127, 128 to 255, ...) at most 5 rows name the same one
- route_weights: float32 [32768, 2], P(('ep', 'tp')), may hold values from 0.1 to 0.9
- gate_weight: bfloat16 [64, 2048, 3584], P('ep', None, 'tp'), may hold values from -0.125 to 0.125
- up_weight: bfloat16 [64, 2048, 3584], P('ep', None, 'tp'), may hold values from -0.125 to 0.125
- down_weight: bfloat16 [64, 3584, 2048], P('ep', 'tp'), may hold values from -0.09375 to 0.09375
Outputs:
- attended: bfloat16 [32768, 2048], P('ep', 'tp')
- moe_out: bfloat16 [32768, 2048], P(('ep', 'tp'))
The draws below stay inside these ranges and needn't reach their ends.
Inputs may be any that keep to these rules, and one draw needn't show every extreme that they name: `routes`: in each aligned block of 128 rows (the rows of one device) no expert is named by more than 5 rows; the 2 entries of a row differ.
All inputs are finite; a program needn't handle non-finite values.
Results may differ from the reference program's by a relative error of at most 0.012.
Values may be sent and summed in bfloat16 or wider, within the bound.
A program may use at most 128 MiB of HBM per device.

```python
import math
import jax
import jax.numpy as jnp
import numpy as np
from jax import lax

D = 2048
HEADS = 32
KV_HEADS = 4
HEAD = 64
WINDOW = 128
FFE = 3584
TOP = 2
TOKB_DEV = 128
EXPERTS = 64
CAP = 5
TOKENS_A = 32768
TOKENS_B = 32768
N_TP = 4


def draw_queries(key, part):
    shape = (TOKENS_A, HEADS * HEAD)
    base = jnp.clip(jax.random.normal(jax.random.fold_in(key, 11), shape, jnp.float32), -6.0, 6.0)
    return base.astype(jnp.bfloat16)


def draw_keys_values(key, part):
    shape = (TOKENS_A, KV_HEADS, HEAD)
    keys = jnp.clip(jax.random.normal(jax.random.fold_in(key, 13), shape, jnp.float32), -6.0, 6.0)
    values = jnp.clip(3.0 * jax.random.normal(jax.random.fold_in(key, 17), shape, jnp.float32), -12.0, 12.0)
    return jnp.concatenate([keys, values], axis=2).astype(jnp.bfloat16)


def level_of(rng, shape, pieces, smallest, high):
    factor_of, own = 1.0, jax.random.fold_in(rng, 6)
    for dim, blocks in pieces:
        steps = jnp.exp(jax.random.uniform(jax.random.fold_in(own, dim), (blocks,), jnp.float32, smallest / len(pieces), high / len(pieces)))
        factor_of = factor_of * jnp.repeat(steps, shape[dim] // blocks).reshape([-1 if axis == dim else 1 for axis in range(len(shape))])
    return factor_of


def routed_block(rng, own, number, rows, amount, top, limit, slope):
    sequence = jax.random.permutation(rng, amount)
    heavy_load, common = load_shares(amount, rows * top, limit, slope, True), load_shares(amount, rows * top, limit, slope, False)
    places = jnp.arange(amount)

    def named(lengths, offset_by):
        used = int((lengths > 0).sum())
        fixed = max(1, used // 4)
        passed = fixed + (places - fixed + offset_by * (used - fixed)) % max(1, amount - fixed)
        return jnp.zeros((amount,), jnp.int32).at[sequence[jnp.where(places < fixed, places, passed)]].set(jnp.asarray(lengths, jnp.int32))

    lengths = jnp.where(number % 4 == 0, named(heavy_load, number // 4), named(common, number - number // 4 - 1))
    mixed = jax.random.permutation(jax.random.fold_in(own, 3), amount)
    donor, sink = mixed[0:amount // 2 * 2:2], mixed[1:amount // 2 * 2:2]
    margin = jnp.minimum(lengths[donor] - 1, limit - lengths[sink]) // 2
    margin = jnp.where((donor == sequence[0]) | (sink == sequence[0]) | (lengths[sink] == 0), 0, jnp.maximum(margin, 0))
    passed = jax.random.randint(jax.random.fold_in(own, 4), (amount // 2,), 0, 1 << 20) % (margin + 1)
    lengths = lengths.at[donor].add(-passed).at[sink].add(passed)
    members = jnp.searchsorted(jnp.cumsum(lengths), jnp.arange(rows * top), side="right").astype(jnp.int32)
    table = members.reshape(top, rows).T
    table = table[jax.random.permutation(jax.random.fold_in(own, 1), rows)]
    offset_by = jax.random.randint(jax.random.fold_in(own, 2), (rows, 1), 0, top)
    return jnp.take_along_axis(table, (jnp.arange(top)[None, :] + offset_by) % top, axis=1)


def load_shares(count, total, bound, slope, full):
    portions = [(1 << 20) // math.isqrt(grade ** slope) + 1 for grade in range(1, count + 1)]
    largest = bound if full else min(bound, max(-(-total // count), total * portions[0] // sum(portions)))
    least = 1 if total - largest >= count - 1 else 0
    counts, surplus = [largest] + [least] * (count - 1), total - largest - least * (count - 1)
    while surplus > 0:
        free = [i for i in range(1, count) if counts[i] < largest] or [i for i in range(1, count) if counts[i] < bound]
        pool, budget = sum([portions[i] for i in free]), surplus
        for i in free:
            extra = min(bound - counts[i], max(1, budget * portions[i] // pool), surplus)
            counts[i] = counts[i] + extra
            surplus = surplus - extra
    return np.array(counts)


def centred(rng, shape, width, bound, split=(), kind=jnp.bfloat16):
    entries = jax.random.normal(rng, shape, jnp.float32) * width
    if len(split) > 0:
        entries = level_of(rng, shape, split, -0.22, 0.18) * entries
    return jnp.clip(entries, min=-bound, max=bound).astype(kind)


def setup_inputs(seed: int = 0) -> dict:
    splits = jax.random.split(jax.random.key(seed), 11)
    queries = draw_queries(jax.random.fold_in(splits[10], 71), 0)
    keys_values = draw_keys_values(jax.random.fold_in(splits[10], 71), 0)
    sinks = jnp.clip(1.0 + 4.0 * jax.random.uniform(splits[2], (HEADS,), jnp.float32) ** level_of(splits[2], (HEADS,), ((0, 4),), -0.2, 0.2), 1.0, 5.0)
    tokens_b = centred(splits[3], (TOKENS_B, D), 1.0, 6.0, ((0, 256),))
    norm_gain = jnp.clip(1.0 + 0.18 * jax.random.normal(splits[4], (D,), jnp.float32), 0.1, 1.9)
    routes_keys = jax.random.split(jax.random.fold_in(splits[5], 1), TOKENS_B // TOKB_DEV)
    routes_turns = jax.random.permutation(jax.random.fold_in(splits[5], 3), TOKENS_B // TOKB_DEV)
    routes = jax.vmap(lambda own, number: routed_block(jax.random.fold_in(splits[5], 2), own, number, TOKB_DEV, EXPERTS, TOP, CAP, 1))(routes_keys, routes_turns).reshape((TOKENS_B, TOP))
    route_weights = jnp.clip(0.1 + 0.79999997 * jax.random.uniform(splits[6], (TOKENS_B, TOP), jnp.float32) ** level_of(splits[6], (TOKENS_B, TOP), ((0, 256),), -0.2, 0.2), 0.1, 0.9)
    gate_weight = centred(splits[7], (EXPERTS, D, FFE), D ** -0.5, 0.125, ((0, 64), (2, 4)))
    up_weight = centred(splits[8], (EXPERTS, D, FFE), D ** -0.5, 0.125, ((0, 64), (2, 4)))
    down_weight = centred(splits[9], (EXPERTS, FFE, D), FFE ** -0.5, 0.09375, ((0, 64), (1, 4)))
    return dict(queries=queries, keys_values=keys_values, sinks=sinks, tokens_b=tokens_b, norm_gain=norm_gain, routes=routes, route_weights=route_weights, gate_weight=gate_weight, up_weight=up_weight, down_weight=down_weight)


NEG_SCORE = -1e+30
EPSILON = 1e-06

def attention_part(queries, keys_values, sinks):
    group_size = HEADS // KV_HEADS
    block_count = TOKENS_A // WINDOW
    padded_kv = jnp.concatenate([jnp.zeros((WINDOW, KV_HEADS, 2 * HEAD), jnp.bfloat16), keys_values], axis=0)
    head_ids = jnp.arange(HEADS, dtype=jnp.float32)
    slopes = (2.0 ** (-8.0 * (head_ids + 1.0) / HEADS)).reshape(KV_HEADS, group_size, 1, 1)
    sink_logit = sinks.reshape(KV_HEADS, group_size, 1, 1)
    query_pos = jnp.arange(WINDOW, dtype=jnp.int32)[:, None]
    key_pos = jnp.arange(2 * WINDOW, dtype=jnp.int32)[None, :]
    distance = WINDOW + query_pos - key_pos

    def one_block(block):
        query_rows = lax.dynamic_slice_in_dim(queries, block * WINDOW, WINDOW, 0)
        query_rows = query_rows.reshape(WINDOW, KV_HEADS, group_size, HEAD).astype(jnp.float32)
        near_kv = lax.dynamic_slice_in_dim(padded_kv, block * WINDOW, 2 * WINDOW, 0).astype(jnp.float32)
        keys = near_kv[:, :, :HEAD]
        values = near_kv[:, :, HEAD:]
        scores = jnp.einsum('qkgd,skd->kgqs', query_rows, keys) * HEAD ** (-0.5)
        key_global = (block - 1) * WINDOW + key_pos
        allowed = (distance >= 0) & (distance < WINDOW) & (key_global >= 0)
        scores = jnp.where(allowed, scores - slopes * distance.astype(jnp.float32), NEG_SCORE)
        peak_score = jnp.maximum(lax.optimization_barrier(jnp.max(scores, axis=-1, keepdims=True)), sink_logit)
        exponent = jnp.exp(scores - peak_score)
        denominator = lax.optimization_barrier(jnp.sum(exponent, axis=-1, keepdims=True)) + jnp.exp(sink_logit - peak_score)
        weights = (exponent / denominator).astype(jnp.bfloat16)
        mixed = jnp.einsum('kgqs,skd->qkgd', weights.astype(jnp.float32), values)
        return mixed.astype(jnp.bfloat16).reshape(WINDOW, HEADS * HEAD)
    blocks_out = lax.map(one_block, jnp.arange(block_count, dtype=jnp.int32))
    return blocks_out.reshape(TOKENS_A, HEADS * HEAD)

def expert_part(tokens_b, norm_gain, routes, route_weights, gate_weight, up_weight, down_weight):
    widened = tokens_b.astype(jnp.float32)
    scale = lax.rsqrt(lax.optimization_barrier(jnp.mean(widened * widened, axis=-1, keepdims=True)) + EPSILON)
    normed = (widened * scale * norm_gain).astype(jnp.bfloat16)
    source_count = TOKENS_B // TOKB_DEV
    pair_count = TOKB_DEV * TOP
    chosen = routes.reshape(source_count, pair_count)
    onehot = (chosen[:, :, None] == jnp.arange(EXPERTS, dtype=jnp.int32)).astype(jnp.int32)
    slots = lax.optimization_barrier(jnp.sum(jnp.cumsum(onehot, axis=1) * onehot, axis=2)) - 1
    row_width = source_count * CAP
    sources = jnp.arange(source_count, dtype=jnp.int32)[:, None]
    destination = chosen * row_width + sources * CAP + slots
    table = jnp.full((EXPERTS * row_width,), source_count * pair_count, jnp.int32)
    table = table.at[destination.reshape(-1)].set(jnp.arange(source_count * pair_count, dtype=jnp.int32))
    table = table.reshape(EXPERTS, row_width)
    flat_weights = jnp.concatenate([route_weights.reshape(-1), jnp.zeros((1,), jnp.float32)])
    padded = jnp.concatenate([normed, jnp.zeros((1, D), jnp.bfloat16)], axis=0)
    local_width = FFE // N_TP

    def expert_step(total, inputs):
        gate_w, up_w, down_w, picks = inputs
        token_ids = picks // TOP
        picked = padded[token_ids]
        gate_part = jnp.dot(picked, gate_w, preferred_element_type=jnp.float32)
        up_part = jnp.dot(picked, up_w, preferred_element_type=jnp.float32)
        hidden = (jax.nn.silu(gate_part) * up_part).astype(jnp.bfloat16)
        parts = jnp.einsum('rjf,jfd->jrd', hidden.reshape(row_width, N_TP, local_width).astype(jnp.float32), down_w.reshape(N_TP, local_width, D).astype(jnp.float32))
        parts = lax.optimization_barrier(parts.astype(jnp.bfloat16)).astype(jnp.float32)
        expert_out = lax.optimization_barrier(jnp.sum(parts, axis=0)).astype(jnp.bfloat16)
        scaled = flat_weights[picks][:, None] * expert_out.astype(jnp.float32)
        return (total.at[token_ids].add(scaled), None)
    start_total = jnp.zeros((TOKENS_B + 1, D), jnp.float32)
    total, _ = lax.scan(expert_step, start_total, (gate_weight, up_weight, down_weight, table))
    return total[:TOKENS_B].astype(jnp.bfloat16)

def reference(queries, keys_values, sinks, tokens_b, norm_gain, routes, route_weights, gate_weight, up_weight, down_weight):
    attended = attention_part(queries, keys_values, sinks)
    moe_out = expert_part(tokens_b, norm_gain, routes, route_weights, gate_weight, up_weight, down_weight)
    return (attended, moe_out)
```

```python
import functools

import jax
import jax.numpy as jnp
from jax import lax
from jax.experimental import pallas as pl
from jax.experimental.pallas import tpu as pltpu
from jax.sharding import PartitionSpec as P

HEADS = 32
WINDOW = 128
NEG_SCORE = -1e30
HEAD = 64
EPSILON = 1e-06
MESH = pl.DeviceIdType.MESH

NX, NC = 4, 2
CAP = 5
N_TP = 4
LANES = 128


PLAN = (
    "A0", "B0", "A1", "C0", "B1", "A2", "D0", "C1", "B2", "A3", "D1", "E0",
    "C2", "B3", "D2", "E1", "C3", "D3", "F0", "E2", "F1", "E3", "F2", "F3",
)


def z_orders(nz):
    return {8: (0, 1, 3, 5, 4, 6, 2, 7), 4: (0, 1, 2, 3), 2: (0, 1)}[nz]


def layer_kernel(
    nz,
    tokens_ref, gain_ref, routes_ref, rw_ref, sinks_ref, q_hbm, kv_hbm, wg_hbm, wu_hbm, wd_hbm,
    moe_ref, att_ref,
    normed, s_ref, out_t, in_t, xg, wg, wu, wd, hidden, part, r1, r2, q1, q2, f1, f2, ret_t, got_t, rows_ref, acc,
    q_ref, kv_ref, key_ref, value_ref,
    w_sem, kv_send, kv_recv, disp_send, disp_recv, ret_send, ret_recv, ag_send, ag_recv, rs_send, rs_recv,
):
    order = z_orders(nz)
    tokens, width = tokens_ref.shape
    half = width // 2
    cols = width // LANES
    ep_size = nz * NX * NC
    group = NX * NC
    chunks = max(1, nz // 2)
    per_chunk = ep_size // chunks
    rows = per_chunk * CAP
    unit = cols
    blk = CAP * unit
    chunk_t = per_chunk * blk
    ffl = wg.shape[1]

    ep = lax.axis_index("ep")
    tp = lax.axis_index("tp")
    my_z, my_x, my_c = ep // group, (ep // NC) % NX, ep % NC
    up_id = {"ep": ep, "tp": (tp + 1) % N_TP}
    dn_id = {"ep": ep, "tp": (tp + N_TP - 1) % N_TP}

    def ep_at(sign, dz, j):
        dx, dc = j // NC, j % NC
        z = (my_z + sign * dz + nz) % nz
        x = (my_x + sign * dx + NX) % NX
        c = (my_c + dc) % NC
        return {"ep": (z * NX + x) * NC + c, "tp": tp}

    def arrived(copy):
        with jax.named_scope("wait"):
            copy.wait_recv()

    barrier = pltpu.get_barrier_semaphore()

    def greet(i, carry):
        pl.semaphore_signal(barrier, inc=1, device_id={"ep": (ep + i) % ep_size, "tp": tp}, device_id_type=MESH)
        return carry

    lax.fori_loop(1, ep_size, greet, 0)
    pl.semaphore_signal(barrier, inc=1, device_id=up_id, device_id_type=MESH)
    pl.semaphore_signal(barrier, inc=1, device_id=dn_id, device_id_type=MESH)

    weight_copies = [
        pltpu.make_async_copy(wg_hbm, wg, w_sem.at[0]),
        pltpu.make_async_copy(wu_hbm, wu, w_sem.at[1]),
        pltpu.make_async_copy(wd_hbm, wd, w_sem.at[2]),
    ]
    kv_rows = kv_hbm.shape[0]
    kv_copy = pltpu.make_async_copy(kv_hbm, kv_ref.at[pl.ds(WINDOW, kv_rows)], w_sem.at[3])
    q_copy = pltpu.make_async_copy(q_hbm, q_ref, w_sem.at[4])
    kv_copy.start()
    q_copy.start()
    before = pltpu.make_async_remote_copy(
        src_ref=kv_ref.at[pl.ds(kv_rows, WINDOW)],
        dst_ref=kv_ref.at[pl.ds(0, WINDOW)],
        send_sem=kv_send,
        recv_sem=kv_recv,
        device_id={"ep": (ep + 1) % ep_size, "tp": tp},
        device_id_type=MESH,
    )

    for copy in weight_copies:
        copy.start()

    widened = tokens_ref[...].astype(jnp.float32)
    scale = lax.rsqrt(jnp.mean(widened * widened, axis=-1, keepdims=True) + EPSILON)
    normed[...] = (widened * scale * gain_ref[...]).astype(jnp.bfloat16)

    def relative_block(e):
        dz = (lax.shift_right_logical(e, 3) - my_z + nz) & (nz - 1)
        dx = ((lax.shift_right_logical(e, 1) & (NX - 1)) - my_x + NX) & (NX - 1)
        dc = ((e & (NC - 1)) + my_c) & (NC - 1)
        pos = jnp.zeros_like(e)
        for q, d in enumerate(order):
            pos = jnp.where(dz == d, q, pos)
        return pos * group + dx * NC + dc

    iota_et = lax.broadcasted_iota(jnp.int32, (LANES, tokens), 0)
    hot_t = [(routes_ref[k : k + 1, :] == iota_et).astype(jnp.float32) for k in range(2)]
    earlier_t = (
        lax.broadcasted_iota(jnp.int32, (tokens, tokens), 0) < lax.broadcasted_iota(jnp.int32, (tokens, tokens), 1)
    ).astype(jnp.bfloat16)
    count_t = jnp.dot((hot_t[0] + hot_t[1]).astype(jnp.bfloat16), earlier_t, preferred_element_type=jnp.float32)
    dest_t = []
    for k in range(2):
        rank = jnp.sum(hot_t[k] * count_t, axis=0, keepdims=True).astype(jnp.int32)
        dest_t.append(relative_block(routes_ref[k : k + 1, :]) * CAP + rank)

    diagonal = lax.broadcasted_iota(jnp.int32, (tokens, tokens), 0) == lax.broadcasted_iota(jnp.int32, (tokens, tokens), 1)

    def as_column(row):
        return jnp.sum(jnp.where(diagonal, row, 0.0), axis=1, keepdims=True)

    dest = [as_column(d.astype(jnp.float32)).astype(jnp.int32) for d in dest_t]
    gains = [as_column(rw_ref[k : k + 1, :]) for k in range(2)]

    col_step = min(512, width)
    groups = col_step // LANES

    def store_tiles(value, start, target, row0):
        for g in range(value.shape[1] // LANES):
            target[pl.ds(row0 + start // LANES + g, rows, stride=unit), :] = value[:, g * LANES : (g + 1) * LANES]

    def send_blocks(c, source, target, sign, send_sem, recv_sem):
        for q in range(2):
            dz = order[2 * c + q]
            first = 1 if dz == 0 else 0

            def one(j, carry, q=q, dz=dz):
                at = pl.multiple_of(((2 * c + q) * group + j) * blk, blk)
                pltpu.make_async_remote_copy(
                    src_ref=source.at[pl.ds(at, blk)],
                    dst_ref=target.at[pl.ds(at, blk)],
                    send_sem=send_sem.at[c],
                    recv_sem=recv_sem.at[c],
                    device_id=ep_at(sign, dz, j),
                    device_id_type=MESH,
                ).start()
                return carry

            lax.fori_loop(first, group, one, 0)
        if order[2 * c] == 0:
            target[c * chunk_t : c * chunk_t + blk, :] = source[c * chunk_t : c * chunk_t + blk, :]

    def chunk_copy(c, source, target, send_sem, recv_sem):
        first = blk if order[2 * c] == 0 else 0
        span = pl.ds(c * chunk_t + first, chunk_t - first)
        return pltpu.make_async_remote_copy(
            src_ref=source.at[span],
            dst_ref=target.at[span],
            send_sem=send_sem.at[c],
            recv_sem=recv_sem.at[c],
            device_id=up_id,
            device_id_type=MESH,
        )

    for c in range(chunks):
        slot = lax.broadcasted_iota(jnp.int32, (rows, tokens), 0) + c * rows
        take = ((dest_t[0] == slot) | (dest_t[1] == slot)).astype(jnp.bfloat16)
        for start in range(0, width, col_step):
            picked = jnp.dot(take, normed[:, start : start + col_step], preferred_element_type=jnp.float32)
            store_tiles(picked, start, s_ref, 0)
        out_t[c * chunk_t : (c + 1) * chunk_t, :] = s_ref[...].astype(jnp.bfloat16)
        if c == 0:
            with jax.named_scope("barrier"):
                pl.semaphore_wait(barrier, ep_size - 1 + 2)
        with jax.named_scope("send%d" % c):
            send_blocks(c, out_t, in_t, 1, disp_send, disp_recv)
        if c == 0:
            kv_copy.wait()
            before.start()

    def attention():
        q_copy.wait()
        before.wait_recv()
        wide = kv_ref[...].astype(jnp.float32)
        flip = pltpu.roll(wide, HEAD, 1)
        lane = lax.broadcasted_iota(jnp.int32, wide.shape, 1)
        key_ref[0] = jnp.where(lane < HEAD, wide, 0.0).astype(jnp.bfloat16)
        key_ref[1] = jnp.where(lane >= HEAD, flip, 0.0).astype(jnp.bfloat16)
        value_ref[0] = jnp.where(lane < HEAD, flip, 0.0).astype(jnp.bfloat16)
        value_ref[1] = jnp.where(lane >= HEAD, wide, 0.0).astype(jnp.bfloat16)
        span = 2 * WINDOW
        shape = (WINDOW, span)
        key_pos = lax.broadcasted_iota(jnp.int32, shape, 1)
        distance = WINDOW + lax.broadcasted_iota(jnp.int32, shape, 0) - key_pos
        in_band = (distance >= 0) & (distance < WINDOW)
        distance = distance.astype(jnp.float32)
        pairs = q_ref.shape[1] // LANES

        def one(i, carry):
            n, pair = i // pairs, i % pairs
            rows_at = pl.ds(pl.multiple_of(n * WINDOW, WINDOW), WINDOW)
            keys_at = pl.ds(pl.multiple_of(n * WINDOW, WINDOW), span)
            lanes_at = pl.ds(pl.multiple_of(pair * LANES, LANES), LANES)
            q = q_ref[rows_at, lanes_at]
            first_key = jnp.where(ep * kv_rows + n == 0, WINDOW, 0)
            allowed = in_band & (key_pos >= first_key)
            total = None
            for odd in range(2):
                head = tp * (2 * pairs) + 2 * pair + odd
                power = jnp.full((1, span), (head + 1).astype(jnp.float32) * (-8.0 / HEADS), jnp.float32)
                score = lax.dot_general(
                    q, key_ref[odd, keys_at, :], (((1,), (1,)), ((), ())), preferred_element_type=jnp.float32
                ) * HEAD ** (-0.5)
                score = jnp.where(allowed, score - jnp.exp2(power) * distance, NEG_SCORE)
                sink = sinks_ref[2 * pair + odd]
                peak = jnp.maximum(jnp.max(score, axis=1, keepdims=True), sink)
                exponent = jnp.exp(score - peak)
                denominator = jnp.sum(exponent, axis=1, keepdims=True) + jnp.exp(sink - peak)
                weight = (exponent * (1.0 / denominator)).astype(jnp.bfloat16)
                mixed = jnp.dot(weight, value_ref[odd, keys_at, :], preferred_element_type=jnp.float32)
                total = mixed if total is None else total + mixed
            att_ref[rows_at, lanes_at] = total.astype(jnp.bfloat16)
            return carry

        lax.fori_loop(0, (kv_rows // WINDOW) * pairs, one, 0)

    def y_copy(source, target, sems, at, device):
        send, recv = sems
        return pltpu.make_async_remote_copy(
            src_ref=source, dst_ref=target, send_sem=send.at[at], recv_sem=recv.at[at],
            device_id=device, device_id_type=MESH,
        )

    AG, RS = (ag_send, ag_recv), (rs_send, rs_recv)
    LOW, HIGH = pl.ds(0, half), pl.ds(half, half)

    def ag_up(c):
        return y_copy(xg.at[c, 0], xg.at[c, 1], AG, 4 * c, up_id)

    def ag_dn(c):
        return y_copy(xg.at[c, 0], xg.at[c, 3], AG, 4 * c + 1, dn_id)

    def ag_up2(c):
        return y_copy(xg.at[c, 1, :, LOW], xg.at[c, 2, :, LOW], AG, 4 * c + 2, up_id)

    def ag_dn2(c):
        return y_copy(xg.at[c, 3, :, HIGH], xg.at[c, 2, :, HIGH], AG, 4 * c + 3, dn_id)

    def rs_far_up(c):
        return y_copy(part.at[c, 2, :, LOW], r1.at[c], RS, 6 * c, up_id)

    def rs_far_dn(c):
        return y_copy(part.at[c, 2, :, HIGH], r2.at[c], RS, 6 * c + 1, dn_id)

    def rs_own_up(c):
        return y_copy(part.at[c, 3, :, HIGH], f1.at[c, 1], RS, 6 * c + 2, up_id)

    def rs_own_dn(c):
        return y_copy(part.at[c, 1, :, LOW], f2.at[c, 0], RS, 6 * c + 3, dn_id)

    def rs_sum_up(c):
        return y_copy(q1.at[c], f1.at[c, 0], RS, 6 * c + 4, up_id)

    def rs_sum_dn(c):
        return y_copy(q2.at[c], f2.at[c, 1], RS, 6 * c + 5, dn_id)

    def stage_a(c):
        arrived(chunk_copy(c, out_t, in_t, disp_send, disp_recv))
        s_ref[...] = in_t[c * chunk_t : (c + 1) * chunk_t, :].astype(jnp.float32)
        for g in range(cols):
            xg[c, 0, :, g * LANES : (g + 1) * LANES] = s_ref[pl.ds(g, rows, stride=unit), :].astype(jnp.bfloat16)
        ag_up(c).start()
        ag_dn(c).start()

    def stage_b(c):
        arrived(ag_up(c))
        ag_up2(c).start()
        arrived(ag_dn(c))
        ag_dn2(c).start()

    def stage_c(c):
        arrived(ag_up2(c))
        arrived(ag_dn2(c))
        if c == 0:
            weight_copies[0].wait()
            weight_copies[1].wait()

        def gate_up(j, carry):
            at = pl.ds(pl.multiple_of(j * LANES, LANES), LANES)
            both = jnp.concatenate([wg[:, at], wu[:, at]], axis=1)
            value = jnp.dot(
                xg[c].reshape(N_TP * rows, width), both, preferred_element_type=jnp.float32
            )
            gate, up = value[:, :LANES], value[:, LANES:]
            hidden[:, at] = (gate / (1.0 + jnp.exp(-gate)) * up).astype(jnp.bfloat16)
            return carry

        lax.fori_loop(0, ffl // LANES, gate_up, 0)
        if c == 0:
            weight_copies[2].wait()

        step = min(256, width)

        def down(j, carry):
            at = pl.ds(pl.multiple_of(j * step, step), step)
            value = jnp.dot(hidden[...], wd[:, at], preferred_element_type=jnp.float32)
            part[c, :, :, at] = value.astype(jnp.bfloat16).reshape(N_TP, rows, step)
            return carry

        lax.fori_loop(0, width // step, down, 0)
        rs_far_up(c).start()
        rs_far_dn(c).start()
        rs_own_up(c).start()
        rs_own_dn(c).start()

    def stage_d(c):
        arrived(rs_far_up(c))
        q1[c] = (part[c, 3, :, :half].astype(jnp.float32) + r1[c].astype(jnp.float32)).astype(jnp.bfloat16)
        rs_sum_up(c).start()
        arrived(rs_far_dn(c))
        q2[c] = (part[c, 1, :, half:].astype(jnp.float32) + r2[c].astype(jnp.float32)).astype(jnp.bfloat16)
        rs_sum_dn(c).start()

    def stage_e(c):
        arrived(rs_own_up(c))
        arrived(rs_own_dn(c))
        arrived(rs_sum_up(c))
        arrived(rs_sum_dn(c))
        for start in range(0, width, col_step):
            h, at = start // half, start % half
            value = part[c, 0, :, start : start + col_step].astype(jnp.float32)
            value = value + f1[c, h, :, at : at + col_step].astype(jnp.float32)
            value = value + f2[c, h, :, at : at + col_step].astype(jnp.float32)
            store_tiles(value, start, s_ref, 0)
        ret_t[c * chunk_t : (c + 1) * chunk_t, :] = s_ref[...].astype(jnp.bfloat16)
        send_blocks(c, ret_t, got_t, -1, ret_send, ret_recv)

    def stage_f(c, first):
        arrived(chunk_copy(c, ret_t, got_t, ret_send, ret_recv))
        s_ref[...] = got_t[c * chunk_t : (c + 1) * chunk_t, :].astype(jnp.float32)
        for g in range(cols):
            rows_ref[:, g * LANES : (g + 1) * LANES] = s_ref[pl.ds(g, rows, stride=unit), :].astype(jnp.bfloat16)
        slot = lax.broadcasted_iota(jnp.int32, (tokens, rows), 1) + c * rows
        mix = jnp.where(dest[0] == slot, gains[0], 0.0) + jnp.where(dest[1] == slot, gains[1], 0.0)
        high = mix.astype(jnp.bfloat16)
        low = (mix - high.astype(jnp.float32)).astype(jnp.bfloat16)
        for start in range(0, width, col_step):
            picked = rows_ref[:, start : start + col_step]
            value = jnp.dot(high, picked, preferred_element_type=jnp.float32)
            value = value + jnp.dot(low, picked, preferred_element_type=jnp.float32)
            if not first:
                value = value + acc[:, start : start + col_step]
            acc[:, start : start + col_step] = value

    with jax.named_scope("attention"):
        attention()
    if chunks == 4:
        plan = PLAN
    else:
        plan = [s + str(c) for s in "ABCDEF" for c in range(chunks)]
    for step in plan:
        c = int(step[1])
        with jax.named_scope(step):
            if step[0] == "F":
                stage_f(c, c == 0)
            else:
                {"A": stage_a, "B": stage_b, "C": stage_c, "D": stage_d, "E": stage_e}[step[0]](c)
    moe_ref[...] = acc[...].astype(jnp.bfloat16)

    before.wait_send()
    for c in range(chunks):
        chunk_copy(c, out_t, in_t, disp_send, disp_recv).wait_send()
        chunk_copy(c, ret_t, got_t, ret_send, ret_recv).wait_send()
        for copy in (ag_up, ag_dn, ag_up2, ag_dn2, rs_far_up, rs_far_dn, rs_own_up, rs_own_dn, rs_sum_up, rs_sum_dn):
            copy(c).wait_send()


def both_parts(queries, keys_values, sinks, tokens_b, norm_gain, routes, route_weights, wg, wu, wd):
    tokens, width = tokens_b.shape
    kv_rows = keys_values.shape[0]
    ffl = wg.shape[1]
    ep_size = lax.axis_size("ep")
    nz = ep_size // (NX * NC)
    chunks = max(1, nz // 2)
    rows = ep_size // chunks * CAP
    unit = width // LANES
    all_t = ep_size * CAP * unit
    half = width // 2
    bf, f32 = jnp.bfloat16, jnp.float32
    vmem = pl.BlockSpec(memory_space=pltpu.VMEM)
    hbm = pl.BlockSpec(memory_space=pl.ANY)
    dma = pltpu.SemaphoreType.DMA
    return pl.pallas_call(
        functools.partial(layer_kernel, nz),
        out_shape=(jax.ShapeDtypeStruct((tokens, width), bf), jax.ShapeDtypeStruct(queries.shape, bf)),
        in_specs=[vmem] * 4 + [pl.BlockSpec(memory_space=pltpu.SMEM)] + [hbm] * 5,
        out_specs=(vmem, vmem),
        scratch_shapes=[
            pltpu.VMEM((tokens, width), bf),
            pltpu.VMEM((rows * unit, LANES), f32),
            pltpu.VMEM((all_t, LANES), bf),
            pltpu.VMEM((all_t, LANES), bf),
            pltpu.VMEM((chunks, N_TP, rows, width), bf),
            pltpu.VMEM((width, ffl), bf),
            pltpu.VMEM((width, ffl), bf),
            pltpu.VMEM((ffl, width), bf),
            pltpu.VMEM((N_TP * rows, ffl), bf),
            pltpu.VMEM((chunks, N_TP, rows, width), bf),
            pltpu.VMEM((chunks, rows, half), bf),
            pltpu.VMEM((chunks, rows, half), bf),
            pltpu.VMEM((chunks, rows, half), bf),
            pltpu.VMEM((chunks, rows, half), bf),
            pltpu.VMEM((chunks, 2, rows, half), bf),
            pltpu.VMEM((chunks, 2, rows, half), bf),
            pltpu.VMEM((all_t, LANES), bf),
            pltpu.VMEM((all_t, LANES), bf),
            pltpu.VMEM((rows, width), bf),
            pltpu.VMEM((tokens, width), f32),
            pltpu.VMEM(queries.shape, bf),
            pltpu.VMEM((kv_rows + WINDOW, LANES), bf),
            pltpu.VMEM((2, kv_rows + WINDOW, LANES), bf),
            pltpu.VMEM((2, kv_rows + WINDOW, LANES), bf),
            dma((5,)), dma, dma,
            dma((chunks,)), dma((chunks,)), dma((chunks,)), dma((chunks,)),
            dma((4 * chunks,)), dma((4 * chunks,)), dma((6 * chunks,)), dma((6 * chunks,)),
        ],
        compiler_params=pltpu.CompilerParams(
            collective_id=0, has_side_effects=True, vmem_limit_bytes=60 * 1024 * 1024
        ),
        name="layer",
    )(
        tokens_b, norm_gain[None, :], routes.T, route_weights.T, sinks, queries,
        keys_values.reshape(kv_rows, LANES), wg, wu, wd,
    )


def local(
    queries, keys_values, sinks, tokens_b, norm_gain, routes, route_weights, gate_weight, up_weight, down_weight
):
    moe_out, attended = both_parts(
        queries, keys_values, sinks, tokens_b, norm_gain, routes, route_weights,
        gate_weight[0], up_weight[0], down_weight[0],
    )
    return (attended, moe_out)


def solution(mesh):
    in_specs = (
        P("ep", "tp"),
        P("ep", "tp", None),
        P("tp"),
        P(("ep", "tp"), None),
        P(),
        P(("ep", "tp"), None),
        P(("ep", "tp"), None),
        P("ep", None, "tp"),
        P("ep", None, "tp"),
        P("ep", "tp", None),
    )
    out_specs = (P("ep", "tp"), P(("ep", "tp"), None))
    return jax.shard_map(local, mesh=mesh, in_specs=in_specs, out_specs=out_specs, check_vma=False)
```
